32 devices in a mesh: ep: 8 (over z, core), tp: 4 (over y, x).
Axes of the slice: x: 2, y: 2, z: 4, core: 2. Of those that a mesh axis runs over, the one named last changes fastest.
Arguments:
- compressed_query: bfloat16 [1024, 1536], P('ep'), may hold values from -6 to 6
- compressed_key_value: bfloat16 [1024, 512], P('ep'), may hold values from -6 to 6
- rotary_key: bfloat16 [1024, 32], P('ep'), may hold values from -600 to 600
- query_norm_scale: float32 [1536], replicated, may hold values from 0.1 to 1.9
- context_norm_scale: float32 [512], replicated, may hold values from 0.1 to 1.9
- query_plain_weight: bfloat16 [1536, 1024], P(None, 'tp'), may hold values from -0.375 to 0.375
- query_rotary_weight: bfloat16 [1536, 512], P(None, 'tp'), may hold values from -0.375 to 0.375
- key_up_weight: bfloat16 [512, 1024], P(None, 'tp'), may hold values from -0.25 to 0.25
- value_up_weight: bfloat16 [512, 1024], P(None, 'tp'), may hold values from -0.25 to 0.25
- output_weight: bfloat16 [1024, 2048], P(None, 'tp'), may hold values from -0.75 to 0.75
- mixture_input: bfloat16 [1024, 2048], P('ep'), may hold values from -6 to 6
- mixture_gain: float32 [2048], replicated, may hold values from 0.1 to 1.9
- routes: int32 [1024, 2], P('ep'), may hold values from 0 to 7, all different within a row; in each aligned block of 128 rows (0 to 127, 128 to 255, ...) at most 48 rows name the same one
- route_weight: float32 [1024, 2], P('ep'), may hold values from 0.2 to 2
- expert_gate: bfloat16 [8, 2048, 4096], P('ep', None, 'tp'), may hold values from -0.125 to 0.125
- expert_up: bfloat16 [8, 2048, 4096], P('ep', None, 'tp'), may hold values from -0.125 to 0.125
- expert_down: bfloat16 [8, 4096, 2048], P('ep', None, 'tp'), may hold values from -0.09375 to 0.09375
- shared_gate: bfloat16 [2048, 512], P(None, 'tp'), may hold values from -0.125 to 0.125
- shared_up: bfloat16 [2048, 512], P(None, 'tp'), may hold values from -0.125 to 0.125
- shared_down: bfloat16 [512, 2048], P(None, 'tp'), may hold values from -0.25 to 0.25
Outputs:
- attended: bfloat16 [1024, 2048], P('ep', 'tp')
- combined: bfloat16 [1024, 2048], P('ep', 'tp')
The draws below stay inside these ranges and needn't reach their ends.
Inputs may be any that keep to these rules, and one draw needn't show every extreme that they name: `routes`: in the rows of each index of ep, no expert is named more than 48 times, a bound that some block reaches there.
All inputs are finite; a program needn't handle non-finite values.
Results may differ from the reference program's by a relative error of at most 0.012.
The reference program's roundings to bfloat16 on the way count: a program that leaves them out, or rounds other values in their place, can miss the bound.
Values may be sent and summed in bfloat16 or wider, within the bound.
A program may use at most 64 MiB of HBM per device.

```python
import math
import jax
import jax.numpy as jnp
import numpy as np
from jax import lax

D = 2048
HEAD_COUNT = 16
PLAIN_HEAD_SIZE = 64
ROTARY_SIZE = 32
VALUE_HEAD_SIZE = 64
QUERY_RANK = 1536
KEY_VALUE_RANK = 512
EXP_FF = 4096
SH_FF = 512
TOPK = 2
TOK2 = 128
SEQUENCE_LEN1 = 1024
TOKENS2 = 1024
EXPERTS = 8
CAP = 48
N_EP = 8


def draw_rotary_key(key, part):
    base = jax.random.normal(key, (SEQUENCE_LEN1, ROTARY_SIZE), jnp.float32)
    return base.astype(jnp.bfloat16)


def levels(rng, extent, pieces, least, high):
    loudness, own = 1.0, jax.random.fold_in(rng, 6)
    for dim, parts in pieces:
        heights = jnp.exp(jax.random.uniform(jax.random.fold_in(own, dim), (parts,), jnp.float32, least / len(pieces), high / len(pieces)))
        loudness = loudness * jnp.repeat(heights, extent[dim] // parts).reshape([-1 if axis == dim else 1 for axis in range(len(extent))])
    return loudness


def assign_block(rng, own, number, rows, number_of, top, most, lean):
    order = jax.random.permutation(rng, number_of)
    packed, common = load_shares(number_of, rows * top, most, lean, True), load_shares(number_of, rows * top, most, lean, False)
    places = jnp.arange(number_of)

    def named(tallies, offset_by):
        used = int((tallies > 0).sum())
        fixed = max(1, used // 4)
        moved = fixed + (places - fixed + offset_by * (used - fixed)) % max(1, number_of - fixed)
        return jnp.zeros((number_of,), jnp.int32).at[order[jnp.where(places < fixed, places, moved)]].set(jnp.asarray(tallies, jnp.int32))

    tallies = jnp.where(number % 4 == 0, named(packed, number // 4), named(common, number - number // 4 - 1))
    mixed = jax.random.permutation(jax.random.fold_in(own, 3), number_of)
    donor, sink = mixed[0:number_of // 2 * 2:2], mixed[1:number_of // 2 * 2:2]
    room = jnp.minimum(tallies[donor] - 1, most - tallies[sink]) // 2
    room = jnp.where((donor == order[0]) | (sink == order[0]) | (tallies[sink] == 0), 0, jnp.maximum(room, 0))
    moved = jax.random.randint(jax.random.fold_in(own, 4), (number_of // 2,), 0, 1 << 20) % (room + 1)
    tallies = tallies.at[donor].add(-moved).at[sink].add(moved)
    members = jnp.searchsorted(jnp.cumsum(tallies), jnp.arange(rows * top), side="right").astype(jnp.int32)
    listing = members.reshape(top, rows).T
    listing = listing[jax.random.permutation(jax.random.fold_in(own, 1), rows)]
    offset_by = jax.random.randint(jax.random.fold_in(own, 2), (rows, 1), 0, top)
    return jnp.take_along_axis(listing, (jnp.arange(top)[None, :] + offset_by) % top, axis=1)


def load_shares(count, total, limit, slope, full):
    loads = [(1 << 20) // math.isqrt(grade ** slope) + 1 for grade in range(1, count + 1)]
    largest = limit if full else min(limit, max(-(-total // count), total * loads[0] // sum(loads)))
    least = 1 if total - largest >= count - 1 else 0
    given, surplus = [largest] + [least] * (count - 1), total - largest - least * (count - 1)
    while surplus > 0:
        candidates = [i for i in range(1, count) if given[i] < largest] or [i for i in range(1, count) if given[i] < limit]
        pool, remaining = sum([loads[i] for i in candidates]), surplus
        for i in candidates:
            addition = min(limit - given[i], max(1, remaining * loads[i] // pool), surplus)
            given[i] = given[i] + addition
            surplus = surplus - addition
    return np.array(given)


def noise(own_key, extent, deviation, bound, cuts=(), kind=jnp.bfloat16):
    factor_of = levels(own_key, extent, cuts, -0.22, 0.18) if cuts else 1.0
    result = jax.random.normal(own_key, extent, jnp.float32) * deviation * factor_of
    return jnp.minimum(jnp.maximum(result, -bound), bound).astype(kind)


def setup_inputs(seed: int = 0) -> dict:
    arg_keys = jax.random.split(jax.random.key(seed), 21)
    compressed_query = noise(arg_keys[0], (SEQUENCE_LEN1, QUERY_RANK), 1.0, 6.0, ((0, 8),))
    compressed_key_value = noise(arg_keys[1], (SEQUENCE_LEN1, KEY_VALUE_RANK), 1.0, 6.0, ((0, 8),))
    rotary_key = draw_rotary_key(jax.random.fold_in(arg_keys[20], 71), 0)
    query_norm_scale = jnp.clip(1.0 + 0.18 * jax.random.normal(arg_keys[3], (QUERY_RANK,), jnp.float32), 0.1, 1.9)
    context_norm_scale = jnp.clip(1.0 + 0.18 * jax.random.normal(arg_keys[4], (KEY_VALUE_RANK,), jnp.float32), 0.1, 1.9)
    query_plain_weight = noise(arg_keys[5], (QUERY_RANK, HEAD_COUNT * PLAIN_HEAD_SIZE), (QUERY_RANK // 6) ** -0.5, 0.375, ((1, 4),))
    query_rotary_weight = noise(arg_keys[6], (QUERY_RANK, HEAD_COUNT * ROTARY_SIZE), (QUERY_RANK // 6) ** -0.5, 0.375, ((1, 4),))
    key_up_weight = noise(arg_keys[7], (KEY_VALUE_RANK, HEAD_COUNT * PLAIN_HEAD_SIZE), KEY_VALUE_RANK ** -0.5, 0.25, ((1, 4),))
    value_up_weight = noise(arg_keys[8], (KEY_VALUE_RANK, HEAD_COUNT * VALUE_HEAD_SIZE), KEY_VALUE_RANK ** -0.5, 0.25, ((1, 4),))
    output_weight = noise(arg_keys[9], (HEAD_COUNT * VALUE_HEAD_SIZE, D), (HEAD_COUNT * VALUE_HEAD_SIZE // 16) ** -0.5, 0.75, ((1, 4),))
    mixture_input = noise(arg_keys[10], (TOKENS2, D), 1.0, 6.0, ((0, 8),))
    mixture_gain = jnp.clip(1.0 + 0.18 * jax.random.normal(arg_keys[11], (D,), jnp.float32), 0.1, 1.9)
    routes_keys = jax.random.split(jax.random.fold_in(arg_keys[12], 1), TOKENS2 // TOK2)
    routes_turns = jax.random.permutation(jax.random.fold_in(arg_keys[12], 3), TOKENS2 // TOK2)
    routes = jax.vmap(lambda own, number: assign_block(jax.random.fold_in(arg_keys[12], 2), own, number, TOK2, EXPERTS, TOPK, CAP, 1))(routes_keys, routes_turns).reshape((TOKENS2, TOPK))
    route_weight = jnp.clip(0.2 + 1.8 * jax.random.uniform(arg_keys[13], (TOKENS2, TOPK), jnp.float32) ** levels(arg_keys[13], (TOKENS2, TOPK), ((0, 8),), -0.2, 0.2), 0.2, 2.0)
    expert_gate = noise(arg_keys[14], (EXPERTS, D, EXP_FF), D ** -0.5, 0.125, ((0, 8), (2, 4)))
    expert_up = noise(arg_keys[15], (EXPERTS, D, EXP_FF), D ** -0.5, 0.125, ((0, 8), (2, 4)))
    expert_down = noise(arg_keys[16], (EXPERTS, EXP_FF, D), EXP_FF ** -0.5, 0.09375, ((0, 8), (2, 4)))
    shared_gate = noise(arg_keys[17], (D, SH_FF), D ** -0.5, 0.125, ((1, 4),))
    shared_up = noise(arg_keys[18], (D, SH_FF), D ** -0.5, 0.125, ((1, 4),))
    shared_down = noise(arg_keys[19], (SH_FF, D), SH_FF ** -0.5, 0.25, ((1, 4),))
    return dict(compressed_query=compressed_query, compressed_key_value=compressed_key_value, rotary_key=rotary_key, query_norm_scale=query_norm_scale, context_norm_scale=context_norm_scale, query_plain_weight=query_plain_weight, query_rotary_weight=query_rotary_weight, key_up_weight=key_up_weight, value_up_weight=value_up_weight, output_weight=output_weight, mixture_input=mixture_input, mixture_gain=mixture_gain, routes=routes, route_weight=route_weight, expert_gate=expert_gate, expert_up=expert_up, expert_down=expert_down, shared_gate=shared_gate, shared_up=shared_up, shared_down=shared_down)


def normed_rows(values, scaling):
    floats = values.astype(jnp.float32)
    return floats * lax.rsqrt(lax.optimization_barrier(jnp.mean(floats * floats, axis=-1, keepdims=True)) + 1e-06) * scaling

def rotary_tables(positions):
    inverse = 1.0 / 10000.0 ** (jnp.arange(0, ROTARY_SIZE, 2, dtype=jnp.float32) / ROTARY_SIZE)
    angles = positions.astype(jnp.float32)[:, None] * inverse[None, :]
    return (jnp.cos(angles), jnp.sin(angles))

def rotate(vectors, cosine, sine_part):
    half_width = vectors.shape[-1] // 2
    front_half = vectors[..., :half_width]
    back_half = vectors[..., half_width:]
    return jnp.concatenate([front_half * cosine - back_half * sine_part, front_half * sine_part + back_half * cosine], axis=-1)

def reference(compressed_query, compressed_key_value, rotary_key, query_norm_scale, context_norm_scale, query_plain_weight, query_rotary_weight, key_up_weight, value_up_weight, output_weight, mixture_input, mixture_gain, routes, route_weight, expert_gate, expert_up, expert_down, shared_gate, shared_up, shared_down):
    positions = jnp.arange(SEQUENCE_LEN1, dtype=jnp.int32)
    cosine, sine_part = rotary_tables(positions)
    compressed = normed_rows(compressed_query, query_norm_scale).astype(jnp.bfloat16)
    query_nope = jnp.dot(compressed, query_plain_weight, preferred_element_type=jnp.float32).astype(jnp.bfloat16)
    query_turn = jnp.dot(compressed, query_rotary_weight, preferred_element_type=jnp.float32).reshape(SEQUENCE_LEN1, HEAD_COUNT, ROTARY_SIZE)
    query_rot = rotate(query_turn, cosine[:, None, :], sine_part[:, None, :])
    context = normed_rows(compressed_key_value, context_norm_scale).astype(jnp.bfloat16)
    key_rot = rotate(rotary_key.astype(jnp.float32), cosine, sine_part)
    key_nope = jnp.dot(context, key_up_weight, preferred_element_type=jnp.float32).astype(jnp.bfloat16)
    value_rows = jnp.dot(context, value_up_weight, preferred_element_type=jnp.float32).astype(jnp.bfloat16)
    scale = (PLAIN_HEAD_SIZE + ROTARY_SIZE) ** (-0.5)
    rows_block = math.gcd(SEQUENCE_LEN1, 512)

    def per_head(inputs):
        head_query, head_turn, head_key, head_value = inputs

        def per_block(block_inputs):
            block_query, block_turn = block_inputs
            scores = (jnp.dot(block_query, head_key.T, preferred_element_type=jnp.float32) + jnp.dot(block_turn, key_rot.T, precision=lax.Precision.HIGHEST)) * scale
            largest = lax.optimization_barrier(jnp.max(scores, axis=-1, keepdims=True))
            weights = jnp.exp(scores - largest)
            summed = jnp.dot(weights.astype(jnp.bfloat16), head_value, preferred_element_type=jnp.float32)
            return (summed / lax.optimization_barrier(jnp.sum(weights, axis=-1, keepdims=True))).astype(jnp.bfloat16)
        blocks = lax.map(per_block, (head_query.reshape(SEQUENCE_LEN1 // rows_block, rows_block, PLAIN_HEAD_SIZE), head_turn.reshape(SEQUENCE_LEN1 // rows_block, rows_block, ROTARY_SIZE)))
        return blocks.reshape(SEQUENCE_LEN1, VALUE_HEAD_SIZE)
    heads_out = lax.map(per_head, (query_nope.reshape(SEQUENCE_LEN1, HEAD_COUNT, PLAIN_HEAD_SIZE).transpose(1, 0, 2), query_rot.transpose(1, 0, 2), key_nope.reshape(SEQUENCE_LEN1, HEAD_COUNT, PLAIN_HEAD_SIZE).transpose(1, 0, 2), value_rows.reshape(SEQUENCE_LEN1, HEAD_COUNT, VALUE_HEAD_SIZE).transpose(1, 0, 2)))
    heads_out = heads_out.transpose(1, 0, 2).reshape(SEQUENCE_LEN1, HEAD_COUNT * VALUE_HEAD_SIZE)
    attended = jnp.dot(heads_out, output_weight, preferred_element_type=jnp.float32).astype(jnp.bfloat16)
    floats = mixture_input.astype(jnp.float32)
    centred = floats - lax.optimization_barrier(jnp.mean(floats, axis=-1, keepdims=True))
    normed = (centred * lax.rsqrt(lax.optimization_barrier(jnp.mean(centred * centred, axis=-1, keepdims=True)) + 1e-05) * mixture_gain).astype(jnp.bfloat16)
    shared_hidden = (jax.nn.silu(jnp.dot(normed, shared_gate, preferred_element_type=jnp.float32)) * jnp.dot(normed, shared_up, preferred_element_type=jnp.float32)).astype(jnp.bfloat16)
    flat_routes = routes.reshape(N_EP, TOK2 * TOPK)
    one_hot = (flat_routes[:, :, None] == jnp.arange(EXPERTS, dtype=jnp.int32)[None, None, :]).astype(jnp.int32)
    ranks = lax.optimization_barrier(jnp.sum(one_hot * (jnp.cumsum(one_hot, axis=1) - 1), axis=-1))
    sources = jnp.arange(N_EP, dtype=jnp.int32)[:, None]
    place = flat_routes * (N_EP * CAP) + sources * CAP + ranks
    token_ids = sources * TOK2 + jnp.arange(TOK2 * TOPK, dtype=jnp.int32)[None, :] // TOPK
    owners = jnp.full((EXPERTS * N_EP * CAP,), TOKENS2, jnp.int32)
    owners = owners.at[place.reshape(-1)].set(token_ids.reshape(-1)).reshape(EXPERTS, N_EP * CAP)
    padded = jnp.concatenate([normed, jnp.zeros((1, D), jnp.bfloat16)], axis=0)

    def per_expert(inputs):
        owner_rows, gate_matrix, up_matrix, down_matrix = inputs
        gathered = padded[owner_rows]
        hidden = (jax.nn.silu(jnp.dot(gathered, gate_matrix, preferred_element_type=jnp.float32)) * jnp.dot(gathered, up_matrix, preferred_element_type=jnp.float32)).astype(jnp.bfloat16)
        return jnp.dot(hidden, down_matrix, preferred_element_type=jnp.float32).astype(jnp.bfloat16)
    results = lax.map(per_expert, (owners, expert_gate, expert_up, expert_down))
    picked = results.reshape(EXPERTS * N_EP * CAP, D)[place.reshape(-1)]
    picked = picked.astype(jnp.float32).reshape(TOKENS2, TOPK, D)
    routed = lax.optimization_barrier(jnp.sum(picked * route_weight[:, :, None], axis=1))
    combined = (jnp.dot(shared_hidden, shared_down, preferred_element_type=jnp.float32) + routed).astype(jnp.bfloat16)
    return (attended, combined)
```

```python
import functools

import jax
import jax.numpy as jnp
from jax import lax
from jax.experimental import pallas as pl
from jax.experimental.pallas import tpu as pltpu
from jax.sharding import PartitionSpec as P

PLAIN = 64
ROT = 32
VALUE = 64
TOPK = 2
F32 = jnp.float32
BF16 = jnp.bfloat16
MESH = pl.DeviceIdType.MESH


def dot(a, b):
    return jnp.dot(a, b, preferred_element_type=F32)


def dot_t(a, b):
    return lax.dot_general(a, b, (((1,), (1,)), ((), ())), preferred_element_type=F32)


def tdot(a, b):
    return lax.dot_general(a, b, (((0,), (0,)), ((), ())), preferred_element_type=F32)


def body(
    E, T, NC,
    cq, ckv, rkt, qscale, cscale, mx, mgain, routes, rweight, cosq, sinq, cosk, sink,
    qp_h, qr_h, ku_h, vu_h, ow_h, gate_h, up_h, down_h, sg_h, su_h, sd_h,
    attended, combined,
    qp, qr, ku, vu, ow, gate, up, down, sg, su, sd,
    normed, outgoing, arr, kv, rk, shared, heads, hidden, rows_out, returned,
    wsem,
    sa, ra, sb, rb, skv, rkv, srk, rrk, ssh, rsh, shd, rhd, sh, rh, sd2, rd2, sr, rr,
):
    ep = lax.axis_index("ep")
    tp = lax.axis_index("tp")
    tx, ty = lax.rem(tp, 2), tp // 2
    xp = ty * 2 + (1 - tx)
    yp = (1 - ty) * 2 + tx
    dg = (1 - ty) * 2 + (1 - tx)
    square = T == 4
    tpeers = (xp, yp, dg) if square else [lax.rem(tp + d, T) for d in range(1, T)]
    eps = [lax.rem(ep + d, E) for d in range(1, E)]
    eps_back = [lax.rem(ep - d + E, E) for d in range(1, E)]
    tokens = mx.shape[0]
    cp = outgoing.shape[1]
    width = outgoing.shape[2]
    slots = E * cp
    ff = gate.shape[1]

    loads = []
    pairs = (
        (sg_h, sg), (su_h, su), (ku_h, ku), (vu_h, vu), (qp_h, qp), (qr_h, qr),
        (gate_h, gate), (up_h, up), (down_h, down), (ow_h, ow), (sd_h, sd),
    )
    for i, (src, dst) in enumerate(pairs):
        load = pltpu.make_async_copy(src, dst, wsem.at[i])
        load.start()
        loads.append(load)
    l_sg, l_su, l_ku, l_vu, l_qp, l_qr, l_gate, l_up, l_down, l_ow, l_sd = loads

    barrier = pltpu.get_barrier_semaphore()
    for e in eps:
        pl.semaphore_signal(barrier, inc=1, device_id=(e, tp), device_id_type=MESH)
    for q in tpeers:
        pl.semaphore_signal(barrier, inc=1, device_id=(ep, q), device_id_type=MESH)

    def remote(src, dst, send, recv, e, q):
        return pltpu.make_async_remote_copy(
            src_ref=src, dst_ref=dst, send_sem=send, recv_sem=recv,
            device_id=(e, q), device_id_type=MESH,
        )

    floats = mx[...].astype(F32)
    centred = floats - jnp.mean(floats, axis=-1, keepdims=True)
    normed[...] = (
        centred
        * lax.rsqrt(jnp.mean(centred * centred, axis=-1, keepdims=True) + 1e-05)
        * mgain[...]
    ).astype(BF16)

    experts = lax.broadcasted_iota(jnp.int32, (E, tokens), 0)
    r0, r1 = routes[0:1, :], routes[1:2, :]
    hit0 = (experts == r0).astype(F32)
    hit1 = (experts == r1).astype(F32)
    before = (
        lax.broadcasted_iota(jnp.int32, (tokens, tokens), 0)
        < lax.broadcasted_iota(jnp.int32, (tokens, tokens), 1)
    ).astype(F32).astype(BF16)
    ranks = dot((hit0 + hit1).astype(BF16), before)
    slot0 = r0 * cp + jnp.sum(hit0 * ranks, axis=0, keepdims=True).astype(jnp.int32)
    slot1 = r1 * cp + jnp.sum(hit1 * ranks, axis=0, keepdims=True).astype(jnp.int32)
    places = lax.broadcasted_iota(jnp.int32, (slots, tokens), 0)
    pick0 = (places == slot0).astype(F32)
    pick1 = (places == slot1).astype(F32)
    mine = normed[:, pl.ds(pl.multiple_of(tp * width, width), width)]
    outgoing[...] = dot((pick0 + pick1).astype(BF16), mine).astype(BF16).reshape(E, cp, width)
    arr[tp, ep] = outgoing[ep]

    pl.semaphore_wait(barrier, (E - 1) + (T - 1))

    sends = []
    for e in eps:
        c = remote(outgoing.at[e], arr.at[tp, ep], sa.at[e], ra.at[ep], e, tp)
        c.start()
        sends.append(c)

    def forward(s):
        for q in tpeers:
            c = remote(arr.at[tp, s], arr.at[tp, s], sb.at[q, s], rb.at[tp, s], ep, q)
            c.start()
            sends.append(c)

    forward(ep)

    def rms(values, scaling):
        v = values.astype(F32)
        return (v * lax.rsqrt(jnp.mean(v * v, axis=-1, keepdims=True) + 1e-06) * scaling).astype(BF16)

    context = rms(ckv[...], cscale[...])
    kw = ku.shape[1]
    l_ku.wait()
    kv[ep, :, 0:kw] = dot(context, ku[...]).astype(BF16)
    l_vu.wait()
    kv[ep, :, kw:] = dot(context, vu[...]).astype(BF16)
    rk[ep] = rkt[...]
    for e in eps:
        c = remote(kv.at[ep], kv.at[ep], skv.at[e], rkv.at[ep], e, tp)
        c.start()
        sends.append(c)
        c = remote(rk.at[ep], rk.at[ep], srk.at[e], rrk.at[ep], e, tp)
        c.start()
        sends.append(c)

    l_sg.wait()
    l_su.wait()
    g = dot(normed[...], sg[...])
    shared[tp] = (g / (1.0 + jnp.exp(-g)) * dot(normed[...], su[...])).astype(BF16)
    for q in tpeers:
        c = remote(shared.at[tp], shared.at[tp], ssh.at[q], rsh.at[tp], ep, q)
        c.start()
        sends.append(c)

    for s in eps_back:
        remote(arr.at[tp, s], arr.at[tp, s], sa.at[s], ra.at[s], s, tp).wait_recv()
        forward(s)

    compressed = rms(cq[...], qscale[...])
    l_qp.wait()
    query = dot(compressed, qp[...]).astype(BF16)
    l_qr.wait()
    turn = dot(compressed, qr[...])
    tw = turn.shape[1]
    lane = lax.broadcasted_iota(jnp.int32, turn.shape, 1)
    if tw % 128 == 0:
        swapped = jnp.where(
            lax.rem(lane, ROT) < ROT // 2,
            pltpu.roll(turn, tw - ROT // 2, 1),
            pltpu.roll(turn, ROT // 2, 1),
        )
    else:
        cuts = [turn[:, i:i + ROT // 2] for i in range(0, tw, ROT // 2)]
        swapped = jnp.concatenate([cuts[i + 1 - 2 * (i % 2)] for i in range(len(cuts))], axis=1)
    query_rot = turn * cosq[...] + swapped * sinq[...]

    l_gate.wait()
    l_up.wait()
    per = E // NC
    tile, out_tile = min(256, ff), min(256, down.shape[1])
    crow = per * cp
    half = crow // 2
    for chunk in range(NC):
        for s in range(chunk * per, (chunk + 1) * per):
            for q in tpeers:
                remote(arr.at[q, s], arr.at[q, s], sb.at[q, s], rb.at[q, s], ep, q).wait_recv()

        @pl.loop(0, ff // tile)
        def _(n):
            cols = pl.ds(pl.multiple_of(n * tile, tile), tile)
            g = jnp.zeros((crow, tile), F32)
            u = jnp.zeros((crow, tile), F32)
            for q in range(T):
                x = arr[q, chunk * per:(chunk + 1) * per].reshape(crow, width)
                g += dot(x, gate[q * width:(q + 1) * width, cols])
                u += dot(x, up[q * width:(q + 1) * width, cols])
            hidden[tp, chunk, :, cols] = (g / (1.0 + jnp.exp(-g)) * u).astype(BF16)

        for q in (xp, yp) if square else tpeers:
            c = remote(hidden.at[tp, chunk], hidden.at[tp, chunk], sh.at[q, chunk], rh.at[tp, chunk], ep, q)
            c.start()
            sends.append(c)

    for s in eps_back:
        remote(kv.at[s], kv.at[s], skv.at[s], rkv.at[s], s, tp).wait_recv()
        remote(rk.at[s], rk.at[s], srk.at[s], rrk.at[s], s, tp).wait_recv()
    raw = jnp.concatenate([rk[s].astype(F32) for s in range(E)], axis=1)
    front, back = raw[:ROT // 2], raw[ROT // 2:]
    key_rot = jnp.concatenate(
        [front * cosk[...] - back * sink[...], front * sink[...] + back * cosk[...]], axis=0
    )
    scale = (PLAIN + ROT) ** (-0.5)
    length = E * tokens
    heads_here = kw // PLAIN
    outs = []
    for h in range(heads_here):
        key = kv[:, :, h * PLAIN:(h + 1) * PLAIN].reshape(length, PLAIN)
        value = kv[:, :, kw + h * VALUE:kw + (h + 1) * VALUE].reshape(length, VALUE)
        scores = (
            dot_t(query[:, h * PLAIN:(h + 1) * PLAIN], key)
            + jnp.dot(
                query_rot[:, h * ROT:(h + 1) * ROT], key_rot,
                precision=lax.Precision.HIGHEST, preferred_element_type=F32,
            )
        ) * scale
        weights = jnp.exp(scores - jnp.max(scores, axis=-1, keepdims=True))
        total = jnp.sum(weights, axis=-1, keepdims=True)
        outs.append((dot(weights.astype(BF16), value) / total).astype(BF16))
    heads[tp] = jnp.concatenate(outs, axis=1)

    def relay(chunk):
        remote(hidden.at[yp, chunk], hidden.at[yp, chunk], sh.at[yp, chunk], rh.at[yp, chunk], ep, yp).wait_recv()
        c = remote(
            hidden.at[yp, chunk, pl.ds(0, half)], hidden.at[yp, chunk, pl.ds(0, half)],
            sd2.at[0, chunk], rd2.at[0, chunk], ep, xp,
        )
        c.start()
        sends.append(c)
        remote(hidden.at[xp, chunk], hidden.at[xp, chunk], sh.at[xp, chunk], rh.at[xp, chunk], ep, xp).wait_recv()
        c = remote(
            hidden.at[xp, chunk, pl.ds(half, half)], hidden.at[xp, chunk, pl.ds(half, half)],
            sd2.at[1, chunk], rd2.at[1, chunk], ep, yp,
        )
        c.start()
        sends.append(c)

    if square:
        for chunk in range(NC):
            relay(chunk)
    for q in tpeers:
        c = remote(heads.at[tp], heads.at[tp], shd.at[q], rhd.at[tp], ep, q)
        c.start()
        sends.append(c)

    l_down.wait()
    features = down.shape[1]
    for chunk in range(NC):
        if square:
            remote(
                hidden.at[dg, chunk, pl.ds(0, half)], hidden.at[dg, chunk, pl.ds(0, half)],
                sd2.at[0, chunk], rd2.at[0, chunk], ep, xp,
            ).wait_recv()
            remote(
                hidden.at[dg, chunk, pl.ds(half, half)], hidden.at[dg, chunk, pl.ds(half, half)],
                sd2.at[1, chunk], rd2.at[1, chunk], ep, yp,
            ).wait_recv()
        else:
            for q in tpeers:
                remote(hidden.at[q, chunk], hidden.at[q, chunk], sh.at[q, chunk], rh.at[q, chunk], ep, q).wait_recv()

        @pl.loop(0, features // out_tile)
        def _(n):
            cols = pl.ds(pl.multiple_of(n * out_tile, out_tile), out_tile)
            acc = jnp.zeros((crow, out_tile), F32)
            for q in range(T):
                acc += dot(hidden[q, chunk], down[q * ff:(q + 1) * ff, cols])
            rows_out[chunk * per:(chunk + 1) * per, :, cols] = acc.astype(BF16).reshape(per, cp, out_tile)

        for s in range(chunk * per, (chunk + 1) * per):
            @pl.when(ep != s)
            def _(s=s):
                remote(rows_out.at[s], returned.at[ep], sr.at[s], rr.at[ep], s, tp).start()

    returned[ep] = rows_out[ep]

    for q in tpeers:
        remote(heads.at[q], heads.at[q], shd.at[q], rhd.at[q], ep, q).wait_recv()
        remote(shared.at[q], shared.at[q], ssh.at[q], rsh.at[q], ep, q).wait_recv()
    l_ow.wait()
    hw = heads.shape[2]
    acc = dot(heads[0], ow[0:hw])
    for q in range(1, T):
        acc += dot(heads[q], ow[q * hw:(q + 1) * hw])
    attended[...] = acc.astype(BF16)
    l_sd.wait()
    sw = shared.shape[2]
    acc = dot(shared[0], sd[0:sw])
    for q in range(1, T):
        acc += dot(shared[q], sd[q * sw:(q + 1) * sw])

    for s in eps_back:
        remote(returned.at[s], returned.at[s], sr.at[s], rr.at[s], s, tp).wait_recv()
    back_rows = returned[...].reshape(slots, features)
    routed = jnp.zeros((tokens, features), F32)
    for k, pick in ((0, pick0), (1, pick1)):
        column = jnp.broadcast_to(rweight[k:k + 1, :], (tokens, tokens)).T[:, 0:1]
        routed += tdot(pick.astype(BF16), back_rows) * column
    combined[...] = (acc + routed).astype(BF16)

    for c in sends:
        c.wait_send()
    for s in eps:
        remote(rows_out.at[s], returned.at[ep], sr.at[s], rr.at[ep], s, tp).wait_send()


def per_device(
    E, T,
    compressed_query, compressed_key_value, rotary_key, query_norm_scale, context_norm_scale,
    query_plain_weight, query_rotary_weight, key_up_weight, value_up_weight, output_weight,
    mixture_input, mixture_gain, routes, route_weight, expert_gate, expert_up, expert_down,
    shared_gate, shared_up, shared_down,
):
    tokens = compressed_query.shape[0]
    heads_here = query_plain_weight.shape[1] // PLAIN
    length = tokens * E
    inverse = 1.0 / 10000.0 ** (jnp.arange(0, ROT, 2, dtype=F32) / ROT)
    mine = (lax.axis_index("ep") * tokens + jnp.arange(tokens, dtype=jnp.int32)).astype(F32)
    angles = mine[:, None] * inverse[None, :]
    c, s = jnp.cos(angles), jnp.sin(angles)
    cosq = jnp.tile(jnp.concatenate([c, c], axis=1), (1, heads_here))
    sinq = jnp.tile(jnp.concatenate([-s, s], axis=1), (1, heads_here))
    angles = inverse[:, None] * jnp.arange(length, dtype=jnp.int32).astype(F32)[None, :]
    cosk, sink = jnp.cos(angles), jnp.sin(angles)

    rows = mixture_input.shape[0]
    model = mixture_input.shape[1]
    capacity = rows * TOPK * 3 // (2 * E)
    cp = -(-capacity // 16) * 16
    NC = 2
    width = model // T
    ff = expert_gate.shape[2]
    features = expert_down.shape[2]
    weights = (
        query_plain_weight, query_rotary_weight, key_up_weight, value_up_weight, output_weight,
        expert_gate[0], expert_up[0], expert_down[0], shared_gate, shared_up, shared_down,
    )
    small = (
        compressed_query, compressed_key_value, rotary_key.T, query_norm_scale[None], context_norm_scale[None],
        mixture_input, mixture_gain[None], routes.T, route_weight.T, cosq, sinq, cosk, sink,
    )
    dma = pltpu.SemaphoreType.DMA
    kw = key_up_weight.shape[1]
    sw = shared_gate.shape[1]
    scratch = [pltpu.VMEM(w.shape, BF16) for w in weights] + [
        pltpu.VMEM((rows, model), BF16),
        pltpu.VMEM((E, cp, width), BF16),
        pltpu.VMEM((T, E, cp, width), BF16),
        pltpu.VMEM((E, tokens, 2 * kw), BF16),
        pltpu.VMEM((E, ROT, tokens), BF16),
        pltpu.VMEM((T, rows, sw), BF16),
        pltpu.VMEM((T, tokens, kw), BF16),
        pltpu.VMEM((T, NC, E // NC * cp, ff), BF16),
        pltpu.VMEM((E, cp, features), BF16),
        pltpu.VMEM((E, cp, features), BF16),
        dma((len(weights),)),
        dma((E,)), dma((E,)),
        dma((T, E)), dma((T, E)),
        dma((E,)), dma((E,)),
        dma((E,)), dma((E,)),
        dma((T,)), dma((T,)),
        dma((T,)), dma((T,)),
        dma((T, NC)), dma((T, NC)),
        dma((2, NC)), dma((2, NC)),
        dma((E,)), dma((E,)),
    ]
    vmem = pl.BlockSpec(memory_space=pltpu.VMEM)
    return pl.pallas_call(
        functools.partial(body, E, T, NC),
        out_shape=(
            jax.ShapeDtypeStruct((tokens, output_weight.shape[1]), BF16),
            jax.ShapeDtypeStruct((rows, features), BF16),
        ),
        in_specs=[vmem] * len(small) + [pl.BlockSpec(memory_space=pl.ANY)] * len(weights),
        out_specs=(vmem, vmem),
        scratch_shapes=scratch,
        compiler_params=pltpu.CompilerParams(
            collective_id=0, has_side_effects=True, vmem_limit_bytes=56 * 1024 * 1024
        ),
    )(*small, *weights)


def solution(mesh):
    row, col = P("ep", None), P(None, "tp")
    three = P("ep", None, "tp")
    in_specs = (
        row, row, row, P(), P(), col, col, col, col, col,
        row, P(), row, row, three, three, three, col, col, col,
    )
    return jax.shard_map(
        functools.partial(per_device, mesh.shape["ep"], mesh.shape["tp"]),
        mesh=mesh, in_specs=in_specs, out_specs=(P("ep", "tp"), P("ep", "tp")), check_vma=False,
    )
```
